128 devices in a mesh: rep: 2 (over z_hi), fs: 32 (over z_lo, y, x), tp: 2 (over core).
Axes of the slice: x: 4, y: 4, z: 4 (z_hi: 2, z_lo: 2; z = z_hi * 2 + z_lo), core: 2. Of those that a mesh axis runs over, the one named last changes fastest.
Arguments:
- resid: bfloat16 [49152, 2048], P(('rep', 'fs', 'tp')), may hold values from -6 to 6
- mix_gain: float32 [2048], replicated, may hold values from 0.1 to 1.9
- query_weight: bfloat16 [2048, 1024], P('fs', 'tp'), may hold values from -0.125 to 0.125
- key_weight: bfloat16 [2048, 1024], P('fs', 'tp'), may hold values from -0.125 to 0.125
- value_weight: bfloat16 [2048, 2048], P('fs', 'tp'), may hold values from -0.125 to 0.125
- head_gain: float32 [2048], P('tp'), may hold values from 0.1 to 1.9
- out_weight: bfloat16 [2048, 2048], P('tp', 'fs'), may hold values from -0.125 to 0.125
- mlp_gain: float32 [2048], replicated, may hold values from 0.1 to 1.9
- gate_weight: bfloat16 [2048, 2816], P('fs', 'tp'), may hold values from -0.125 to 0.125
- up_weight: bfloat16 [2048, 2816], P('fs', 'tp'), may hold values from -0.125 to 0.125
- down_weight: bfloat16 [2816, 2048], P('tp', 'fs'), may hold values from -0.109375 to 0.109375
Outputs:
- layer_out: bfloat16 [49152, 2048], P(('rep', 'fs', 'tp'))
The draws below stay inside these ranges and needn't reach their ends.
All inputs are finite; a program needn't handle non-finite values.
Results may differ from the reference program's by a relative error of at most 0.014.
Values may be sent and summed in bfloat16 or wider, within the bound.
No kernel may reach another device: no remote copies, remote signals or barrier semaphores. Data moves between devices by JAX's collectives and lax.ppermute only.
A program may use at most 128 MiB of HBM per device.

```python
import jax
import jax.numpy as jnp
from jax import lax

D = 2048
HEADS = 4
DK = 256
DV = 512
FF = 2816
BLOCK = 128
LEN = 768
TOKENS = 49152
N_TP = 2


def shard_levels(own_key, shape, pieces, least, top_value):
    def one(dim, parts):
        heights = jax.random.uniform(jax.random.fold_in(jax.random.fold_in(own_key, 6), dim), (parts,), jnp.float32, least / len(pieces), top_value / len(pieces))
        return jnp.repeat(jnp.exp(heights), shape[dim] // parts).reshape((-1,) + (1,) * (len(shape) - dim - 1))

    level = one(*pieces[0])
    for cut in pieces[1:]:
        level = level * one(*cut)
    return level


def noise(stream_key, dims, spread, reach, split=(), held_as=jnp.bfloat16):
    level = shard_levels(stream_key, dims, split, -0.22, 0.18) if split else 1.0
    entries = jax.random.normal(stream_key, dims, jnp.float32) * spread * level
    return jnp.minimum(jnp.maximum(entries, -reach), reach).astype(held_as)


def setup_inputs(seed: int = 0) -> dict:
    arg_keys = jax.random.split(jax.random.key(seed), 12)
    resid = noise(arg_keys[0], (TOKENS, D), 1.0, 6.0, ((0, 128),))
    mix_gain = jnp.clip(1.0 + 0.18 * jax.random.normal(arg_keys[1], (D,), jnp.float32), 0.1, 1.9)
    query_weight = noise(arg_keys[2], (D, HEADS * DK), D ** -0.5, 0.125, ((0, 32), (1, 2)))
    key_weight = noise(arg_keys[3], (D, HEADS * DK), D ** -0.5, 0.125, ((0, 32), (1, 2)))
    value_weight = noise(arg_keys[4], (D, HEADS * DV), D ** -0.5, 0.125, ((0, 32), (1, 2)))
    head_gain = jnp.clip(1.0 + 0.18 * jax.random.normal(arg_keys[5], (HEADS * DV,), jnp.float32), 0.1, 1.9)
    out_weight = noise(arg_keys[6], (HEADS * DV, D), (HEADS * DV) ** -0.5, 0.125, ((0, 2), (1, 32)))
    mlp_gain = jnp.clip(1.0 + 0.18 * jax.random.normal(arg_keys[7], (D,), jnp.float32), 0.1, 1.9)
    gate_weight = noise(arg_keys[8], (D, FF), D ** -0.5, 0.125, ((0, 32), (1, 2)))
    up_weight = noise(arg_keys[9], (D, FF), D ** -0.5, 0.125, ((0, 32), (1, 2)))
    down_weight = noise(arg_keys[10], (FF, D), FF ** -0.5, 0.109375, ((0, 2), (1, 32)))
    return {"resid": resid, "mix_gain": mix_gain, "query_weight": query_weight, "key_weight": key_weight, "value_weight": value_weight, "head_gain": head_gain, "out_weight": out_weight, "mlp_gain": mlp_gain, "gate_weight": gate_weight, "up_weight": up_weight, "down_weight": down_weight}


norm_eps = 1e-06
rope_base = 10000.0

def stored(values):
    return lax.optimization_barrier(values.astype(jnp.bfloat16)).astype(jnp.float32)

def rms_scale(values, gain):
    widened = values.astype(jnp.float32)
    scaled = widened * lax.rsqrt(lax.optimization_barrier(jnp.mean(widened * widened, axis=-1, keepdims=True)) + norm_eps)
    return (scaled * gain.astype(jnp.float32)).astype(jnp.bfloat16)

def rotate(vectors):
    length_total = vectors.shape[0]
    half_width = vectors.shape[-1] // 2
    position = jnp.arange(length_total, dtype=jnp.float32)
    inverse = 1.0 / rope_base ** jnp.linspace(0.0, 1.0, half_width, dtype=jnp.float32)
    angle = position[:, None] * inverse[None, :]
    cosine = jnp.cos(angle)[:, None, :]
    sine = jnp.sin(angle)[:, None, :]
    first = vectors[..., :half_width]
    second = vectors[..., half_width:]
    return jnp.concatenate([first * cosine - second * sine, second * cosine + first * sine], axis=-1)

def decay_tables(head_ids, block):
    log_gamma = jnp.log1p(-2.0 ** (-5.0 - 2.0 * head_ids.astype(jnp.float32)))
    offset = jnp.arange(block, dtype=jnp.float32)
    distance = offset[:, None] - offset[None, :]
    inside = jnp.where(distance >= 0, jnp.exp(log_gamma[:, None, None] * jnp.maximum(distance, 0.0)), 0.0)
    query_decay = jnp.exp(log_gamma[:, None] * (offset + 1.0))
    key_decay = jnp.exp(log_gamma[:, None] * (block - 1.0 - offset))
    block_decay = jnp.exp(log_gamma * block)
    return (inside, query_decay, key_decay, block_decay)

def retain(queries, keys, values, head_ids, block):
    length_total, heads, key_width = queries.shape
    value_width = values.shape[-1]
    count = length_total // block
    inside, query_decay, key_decay, block_decay = decay_tables(head_ids, block)

    def blocks(tensor):
        return tensor.reshape(count, block, heads, tensor.shape[-1]).transpose(0, 2, 1, 3)

    def advance(memory, inputs):
        query_tile_rows, key_tile_rows, value_block = inputs
        query_widened = query_tile_rows.astype(jnp.float32)
        value_wide = value_block.astype(jnp.float32)
        attention_scores = jnp.einsum('zvf,zjf->zvj', query_widened, key_tile_rows.astype(jnp.float32))
        weights = stored(attention_scores * inside)
        within = jnp.einsum('hlm,hmv->hlv', weights, value_wide)
        carried = jnp.einsum('hld,hdv->hlv', query_widened, stored(memory)) * query_decay[:, :, None]
        weighted_keys = stored(key_tile_rows.astype(jnp.float32) * key_decay[:, :, None])
        memory = memory * block_decay[:, None, None] + jnp.einsum('hld,hlv->hdv', weighted_keys, value_wide)
        return (memory, within + carried)
    start_state = jnp.zeros((heads, key_width, value_width), jnp.float32)
    _, outputs = lax.scan(advance, start_state, (blocks(queries), blocks(keys), blocks(values)))
    return outputs.transpose(0, 2, 1, 3).reshape(length_total, heads, value_width)

def head_scale(retained, gain):
    scaled = retained * lax.rsqrt(lax.optimization_barrier(jnp.mean(retained * retained, axis=-1, keepdims=True)) + norm_eps)
    return (scaled.reshape(retained.shape[0], -1) * gain.astype(jnp.float32)).astype(jnp.bfloat16)

def reference(resid, mix_gain, query_weight, key_weight, value_weight, head_gain, out_weight, mlp_gain, gate_weight, up_weight, down_weight):
    head_ids = jnp.arange(HEADS, dtype=jnp.int32)
    head_share = HEADS * DV // N_TP
    unit_share = FF // N_TP

    def single_sequence(token_rows):
        normed = rms_scale(token_rows, mix_gain)
        queries = stored(jnp.dot(normed, query_weight, preferred_element_type=jnp.float32)).reshape(LEN, HEADS, DK)
        keys = stored(jnp.dot(normed, key_weight, preferred_element_type=jnp.float32)).reshape(LEN, HEADS, DK)
        values = jnp.dot(normed, value_weight, preferred_element_type=jnp.float32).astype(jnp.bfloat16)
        values = values.reshape(LEN, HEADS, DV)
        query_rot = rotate(queries).astype(jnp.bfloat16)
        key_rot = (rotate(keys) * DK ** (-0.5)).astype(jnp.bfloat16)
        retained = retain(query_rot, key_rot, values, head_ids, BLOCK)
        head_out = head_scale(retained, head_gain)
        mixer_sum = jnp.zeros((LEN, D), jnp.float32)
        for group in range(N_TP):
            lower = group * head_share
            partial_sum = jnp.dot(head_out[:, lower:lower + head_share], out_weight[lower:lower + head_share], preferred_element_type=jnp.float32)
            mixer_sum = mixer_sum + stored(partial_sum)
        middle = (token_rows.astype(jnp.float32) + mixer_sum).astype(jnp.bfloat16)
        normed_mlp = rms_scale(middle, mlp_gain)
        gate = jnp.dot(normed_mlp, gate_weight, preferred_element_type=jnp.float32)
        upward = jnp.dot(normed_mlp, up_weight, preferred_element_type=jnp.float32)
        hidden_units = (jax.nn.silu(gate) * upward).astype(jnp.bfloat16)
        mlp_sum = jnp.zeros((LEN, D), jnp.float32)
        for group in range(N_TP):
            lower = group * unit_share
            partial_sum = jnp.dot(hidden_units[:, lower:lower + unit_share], down_weight[lower:lower + unit_share], preferred_element_type=jnp.float32)
            mlp_sum = mlp_sum + stored(partial_sum)
        return (middle.astype(jnp.float32) + mlp_sum).astype(jnp.bfloat16)
    sequences = resid.reshape(TOKENS // LEN, LEN, D)
    return lax.map(single_sequence, sequences).reshape(TOKENS, D)
```

```python
import jax
import jax.numpy as jnp
from jax import lax
from jax.sharding import Mesh
from jax.sharding import PartitionSpec as P

DK = 256
DV = 512
BLOCK = 128
FS = ("fs_0", "fs_1", "fs_2")
REP_FS_TP = ("rep", "fs_0", "fs_1", "fs_2", "tp")


norm_eps = 1e-06
rope_base = 10000.0


TORUS = ("rep", "fs_0", "fs_1", "fs_2")


def with_partner(shard):
    other = lax.ppermute(shard, "tp", ((0, 1), (1, 0)))
    first = lax.axis_index("tp") == 0
    return jnp.concatenate([jnp.where(first, shard, other), jnp.where(first, other, shard)], axis=0)


def sum_at_owner(partial):
    rows = partial.shape[0] // 2
    index = lax.axis_index("tp")
    mine = lax.dynamic_slice_in_dim(partial, index * rows, rows, 0)
    away = lax.dynamic_slice_in_dim(partial, (1 - index) * rows, rows, 0)
    arrived = lax.ppermute(away, "tp", ((0, 1), (1, 0)))
    return mine.astype(jnp.float32) + arrived.astype(jnp.float32)


def half_of(first, second):
    return jnp.where(lax.axis_index("rep") == 0, first, second)


def rms_scale(values, gain):
    widened = values.astype(jnp.float32)
    scaled = widened * lax.rsqrt(jnp.mean(widened * widened, axis=-1, keepdims=True) + norm_eps)
    return (scaled * gain).astype(jnp.bfloat16)


def rotate(vectors):
    length_total = vectors.shape[0]
    half_width = vectors.shape[-1] // 2
    position = jnp.arange(length_total, dtype=jnp.float32)
    inverse = 1.0 / rope_base ** jnp.linspace(0.0, 1.0, half_width, dtype=jnp.float32)
    angle = position[:, None] * inverse[None, :]
    cosine = jnp.cos(angle)[:, None, :]
    sine = jnp.sin(angle)[:, None, :]
    first = vectors[..., :half_width]
    second = vectors[..., half_width:]
    return jnp.concatenate(
        [first * cosine - second * sine, second * cosine + first * sine], axis=-1
    )


def decay_tables(head_ids, block):
    log_gamma = jnp.log1p(-(2.0 ** (-5.0 - 2.0 * head_ids.astype(jnp.float32))))
    offset = jnp.arange(block, dtype=jnp.float32)
    distance = offset[:, None] - offset[None, :]
    inside = jnp.where(
        distance >= 0, jnp.exp(log_gamma[:, None, None] * jnp.maximum(distance, 0.0)), 0.0
    )
    query_decay = jnp.exp(log_gamma[:, None] * (offset + 1.0))
    key_decay = jnp.exp(log_gamma[:, None] * (block - 1.0 - offset))
    block_decay = jnp.exp(log_gamma * block)
    return (inside, query_decay, key_decay, block_decay)


def retain(queries, keys, values, head_ids, block):
    length_total, heads, key_width = queries.shape
    value_width = values.shape[-1]
    count = length_total // block
    inside, query_decay, key_decay, block_decay = decay_tables(head_ids, block)

    def blocks(tensor):
        return tensor.reshape(count, block, heads, tensor.shape[-1]).transpose(0, 2, 1, 3)

    def advance(memory, inputs):
        query_tile_rows, key_tile_rows, value_block = inputs
        attention_scores = jnp.einsum(
            "zvf,zjf->zvj", query_tile_rows, key_tile_rows, preferred_element_type=jnp.float32
        )
        weights = (attention_scores * inside).astype(jnp.bfloat16)
        within = jnp.einsum(
            "hlm,hmv->hlv", weights, value_block, preferred_element_type=jnp.float32
        )
        carried = (
            jnp.einsum(
                "hld,hdv->hlv",
                query_tile_rows,
                memory.astype(jnp.bfloat16),
                preferred_element_type=jnp.float32,
            )
            * query_decay[:, :, None]
        )
        weighted_keys = (key_tile_rows.astype(jnp.float32) * key_decay[:, :, None]).astype(
            jnp.bfloat16
        )
        memory = memory * block_decay[:, None, None] + jnp.einsum(
            "hld,hlv->hdv", weighted_keys, value_block, preferred_element_type=jnp.float32
        )
        return (memory, within + carried)

    start_state = jnp.zeros((heads, key_width, value_width), jnp.float32)
    _, outputs = lax.scan(advance, start_state, (blocks(queries), blocks(keys), blocks(values)))
    return outputs.transpose(0, 2, 1, 3).reshape(length_total, heads, value_width)


def head_scale(retained, gain):
    scaled = retained * lax.rsqrt(jnp.mean(retained * retained, axis=-1, keepdims=True) + norm_eps)
    return (scaled.reshape(retained.shape[0], -1) * gain).astype(jnp.bfloat16)


def shards(
    resid,
    mix_gain,
    query_weight,
    key_weight,
    value_weight,
    head_gain,
    out_weight,
    mlp_gain,
    gate_weight,
    up_weight,
    down_weight,
):
    token_rows = resid.shape[0]
    length_total = token_rows * lax.axis_size("tp")
    key_cols = query_weight.shape[1]
    heads_here = key_cols // DK
    out_shard = out_weight.T
    down_shard = down_weight.T
    half_out = out_shard.shape[1] // 2
    half_down = down_shard.shape[1] // 2
    first_shard = half_of(
        jnp.concatenate([query_weight, key_weight, out_shard[:, :half_out]], axis=1),
        jnp.concatenate([value_weight, out_shard[:, half_out:]], axis=1),
    )
    second_shard = half_of(
        jnp.concatenate([gate_weight, down_shard[:, :half_down]], axis=1),
        jnp.concatenate([up_weight, down_shard[:, half_down:]], axis=1),
    )
    first_full = lax.all_gather(first_shard, TORUS, axis=0, tiled=True)
    first_full, second_shard = lax.optimization_barrier((first_full, second_shard))
    second_full = lax.all_gather(second_shard, TORUS, axis=0, tiled=True)
    width = first_full.shape[0] // 2

    def dot(a, b):
        return jnp.dot(a, b, preferred_element_type=jnp.float32)

    def dot_t(a, b):
        return lax.dot_general(a, b, (((1,), (1,)), ((), ())), preferred_element_type=jnp.float32)

    normed = with_partner(rms_scale(resid, mix_gain))
    qk = dot(normed, first_full[:width, : 2 * key_cols]).astype(jnp.bfloat16).astype(jnp.float32)
    queries = qk[:, :key_cols].reshape(length_total, heads_here, DK)
    keys = qk[:, key_cols:].reshape(length_total, heads_here, DK)
    values = dot(normed, first_full[width:, : 2 * key_cols]).astype(jnp.bfloat16)
    values = values.reshape(length_total, heads_here, DV)
    query_rot = rotate(queries).astype(jnp.bfloat16)
    key_rot = (rotate(keys) * DK ** (-0.5)).astype(jnp.bfloat16)
    head_ids = lax.axis_index("tp") * heads_here + jnp.arange(heads_here, dtype=jnp.int32)
    retained = retain(query_rot, key_rot, values, head_ids, BLOCK)
    head_out = head_scale(retained, head_gain)
    mixer_sum = sum_at_owner(
        (
            dot_t(head_out[:, :half_out], first_full[:width, 2 * key_cols :])
            + dot_t(head_out[:, half_out:], first_full[width:, 2 * key_cols :])
        ).astype(jnp.bfloat16)
    )
    middle = (resid.astype(jnp.float32) + mixer_sum).astype(jnp.bfloat16)
    normed_mlp = with_partner(rms_scale(middle, mlp_gain))
    units = gate_weight.shape[1]
    gate = dot(normed_mlp, second_full[:width, :units])
    up = dot(normed_mlp, second_full[width:, :units])
    hidden_units = (jax.nn.silu(gate) * up).astype(jnp.bfloat16)
    mlp_sum = sum_at_owner(
        (
            dot_t(hidden_units[:, :half_down], second_full[:width, units:])
            + dot_t(hidden_units[:, half_down:], second_full[width:, units:])
        ).astype(jnp.bfloat16)
    )
    return (middle.astype(jnp.float32) + mlp_sum).astype(jnp.bfloat16)


def solution(mesh):
    torus = Mesh(
        mesh.devices.reshape(mesh.shape["rep"], 2, 4, 4, mesh.shape["tp"]),
        ("rep", "fs_0", "fs_1", "fs_2", "tp"),
    )
    return jax.shard_map(
        shards,
        mesh=torus,
        in_specs=(
            P(REP_FS_TP, None),
            P(),
            P(FS, "tp"),
            P(FS, "tp"),
            P(FS, "tp"),
            P("tp"),
            P("tp", FS),
            P(),
            P(FS, "tp"),
            P(FS, "tp"),
            P("tp", FS),
        ),
        out_specs=P(REP_FS_TP, None),
        check_vma=False,
    )
```

```python
import functools

import jax
import jax.numpy as jnp
from jax import lax
from jax.experimental import pallas as pl
from jax.experimental.pallas import tpu as pltpu
from jax.sharding import Mesh
from jax.sharding import PartitionSpec as P


DK = 256
DV = 512
SPAN = 256
FS = ("fs_0", "fs_1", "fs_2")
TORUS = ("rep", "fs_0", "fs_1", "fs_2")
REP_FS_TP = ("rep", "fs_0", "fs_1", "fs_2", "tp")
X, Y, Z = "fs_2", "fs_1", ("rep", "fs_0")
MIB = 1 << 20


norm_eps = 1e-06
rope_base = 10000.0


def rms_scale(values, gain):
    widened = values.astype(jnp.float32)
    scaled = widened * lax.rsqrt(jnp.mean(widened * widened, axis=-1, keepdims=True) + norm_eps)
    return (scaled * gain).astype(jnp.bfloat16)


def swap(shard):
    return lax.ppermute(shard, "tp", ((0, 1), (1, 0)))


def half_of(first, second):
    return jnp.where(lax.axis_index("rep") == 0, first, second)


def take(block, axis, offset):
    return lax.ppermute(block, axis, [(i, (i - offset) % 4) for i in range(4)])


def ring_x_y_z(shard):
    own = shard[None]
    row = jnp.concatenate([own, take(own, X, 1), take(own, X, 2), take(own, X, 3)], axis=0)
    after, before = take(row, Y, 1), take(row, Y, 3)
    far_a, far_b = take(after[:2], Y, 1), take(before[2:], Y, 3)
    parts = [
        (row, [(0, 0, x) for x in range(4)]),
        (after, [(0, 1, x) for x in range(4)]),
        (before, [(0, 3, x) for x in range(4)]),
        (far_a, [(0, 2, x) for x in range(2)]),
        (far_b, [(0, 2, x) for x in range(2, 4)]),
    ]
    ways = (1, 3, 1, 3, 1)
    return parts + [
        (take(block, Z, way), [(1, y, x) for _, y, x in offsets])
        for (block, offsets), way in zip(parts, ways)
    ]


def ring_z_y_x(shard):
    own = shard[None]
    pair = jnp.concatenate([own, take(own, Z, 1)], axis=0)
    plane = jnp.concatenate([pair, take(pair, Y, 1), take(pair, Y, 2), take(pair, Y, 3)], axis=0)
    offsets = [(z, y) for y in range(4) for z in range(2)]
    after, before = take(plane, X, 1), take(plane, X, 3)
    far_a, far_b = take(after[:4], X, 1), take(before[4:], X, 3)
    return [
        (plane, [(z, y, 0) for z, y in offsets]),
        (after, [(z, y, 1) for z, y in offsets]),
        (before, [(z, y, 3) for z, y in offsets]),
        (far_a, [(z, y, 2) for z, y in offsets[:4]]),
        (far_b, [(z, y, 2) for z, y in offsets[4:]]),
    ]


def positions(parts):
    z, y, x = (lax.axis_index(axis) for axis in FS)
    offsets = jnp.array([offset for _, many in parts for offset in many], jnp.int32)
    return ((z ^ offsets[:, 0]) * 4 + (y + offsets[:, 1]) % 4) * 4 + (x + offsets[:, 2]) % 4


def each_shard(refs):
    shards = [ref.at[i] for ref in refs for i in range(ref.shape[0])]
    return enumerate(shards)


def fetch_rows(own, other, rows, sem, tp):
    mine = pltpu.make_async_copy(own, rows.at[tp], sem)
    theirs = pltpu.make_async_copy(other, rows.at[1 - tp], sem)
    mine.start()
    theirs.start()
    return pltpu.make_async_copy(rows, rows, sem)


def dot(a, b):
    return jnp.dot(a, b, preferred_element_type=jnp.float32)


def dot_t(a, b):
    return lax.dot_general(a, b, (((1,), (1,)), ((), ())), preferred_element_type=jnp.float32)


def retention_body(place, scalars, cosine, sine, gain, own, other, *rest):
    parts, (out, rows, weights, query, key, value, sems, row_sem) = rest[:-8], rest[-8:]
    tp = place[place.shape[0] - 1]
    both = fetch_rows(own, other, rows, row_sem, tp)
    heads = weights.shape[0]
    width = 2 * DK + DV
    for h in range(heads):
        for i, shard in each_shard(parts):
            pltpu.make_async_copy(
                shard.at[:, pl.ds(h * width, width)], weights.at[h, place[i]], sems.at[h]
            ).start()
    both.wait()
    length = rows.shape[0] * rows.shape[1]
    depth = rows.shape[2]
    count = length // SPAN
    row = lax.broadcasted_iota(jnp.int32, (SPAN, SPAN), 0)
    col = lax.broadcasted_iota(jnp.int32, (SPAN, SPAN), 1)

    def turn(vectors, scale):
        vectors = vectors.astype(jnp.bfloat16).astype(jnp.float32)
        first, second = vectors[:, : DK // 2], vectors[:, DK // 2 :]
        c, s = cosine[...], sine[...]
        turned = jnp.concatenate([first * c - second * s, second * c + first * s], axis=1)
        return (turned * scale).astype(jnp.bfloat16) if scale != 1 else turned.astype(jnp.bfloat16)

    def head(h, carry):
        pltpu.make_async_copy(weights.at[h], weights.at[h], sems.at[h]).wait()
        x = rows[...].reshape(length, depth)

        def columns(start, many):
            return weights[h, :, :, start : start + many].reshape(depth, many)

        query[...] = turn(dot(x, columns(0, DK)), 1)
        key[...] = turn(dot(x, columns(DK, DK)), DK ** (-0.5))
        value[...] = dot(x, columns(2 * DK, DV)).astype(jnp.bfloat16)
        log_gamma = scalars[h]
        for i in range(count):
            total = jnp.zeros((SPAN, DV), jnp.float32)
            for j in range(i + 1):
                distance = (row - col + (i - j) * SPAN).astype(jnp.float32)
                decay = jnp.where(distance >= 0, jnp.exp(log_gamma * jnp.maximum(distance, 0.0)), 0.0)
                scores = dot_t(query[i * SPAN : (i + 1) * SPAN], key[j * SPAN : (j + 1) * SPAN])
                total += dot((scores * decay).astype(jnp.bfloat16), value[j * SPAN : (j + 1) * SPAN])
            scaled = total * lax.rsqrt(jnp.mean(total * total, axis=-1, keepdims=True) + norm_eps)
            lanes = pl.ds(pl.multiple_of(h * DV, DV), DV)
            out[i * SPAN : (i + 1) * SPAN, lanes] = (scaled * gain[:, lanes]).astype(jnp.bfloat16)
        return carry

    lax.fori_loop(0, heads, head, 0)


def project_body(place, hidden, *rest):
    parts, (away, mine, weights, sems) = rest[:-4], rest[-4:]
    tp = place[place.shape[0] - 1]
    shards, depth, width = weights.shape
    step = SPAN // depth
    for i, shard in each_shard(parts):
        pltpu.make_async_copy(shard, weights.at[place[i]], sems.at[place[i] // step]).start()
    multiply(tp, hidden, away, mine, weights, sems, step)


def multiply(tp, hidden, away, mine, weights, sems, step):
    shards, depth, width = weights.shape
    half = away.shape[0]

    def block(n, carry):
        some = weights.at[pl.ds(n * step, step)]
        pltpu.make_async_copy(some, some, sems.at[n]).wait()
        right = weights[pl.ds(n * step, step)].reshape(step * depth, width)
        first = hidden[pl.ds(pl.multiple_of((1 - tp) * half, half), half), :]
        second = hidden[pl.ds(pl.multiple_of(tp * half, half), half), :]
        result = dot_t(jnp.concatenate([first, second], axis=0), right).astype(jnp.bfloat16)
        lanes = pl.ds(pl.multiple_of(n * SPAN, SPAN), SPAN)
        away[:, lanes] = result[:half]
        mine[:, lanes] = result[half:]
        return carry

    lax.fori_loop(0, shards // step, block, 0)


def feed_forward_body(place, own, other, full, away, mine, rows, gate, up, hidden, down, row_sem, sems, down_sems):
    tp = place[place.shape[0] - 1]
    both = fetch_rows(own, other, rows, row_sem, tp)
    units = gate.shape[2]
    groups = sems.shape[0]
    tall = gate.shape[1]
    cuts = [min(units, 384 * g) for g in range(groups + 1)]
    for g in range(groups):
        lanes = pl.ds(cuts[g], cuts[g + 1] - cuts[g])
        for side, target in enumerate((gate, up)):
            pltpu.make_async_copy(
                full.at[side, :, pl.ds(0, tall), lanes], target.at[:, :, lanes], sems.at[g, side]
            ).start()
    short = full.shape[2] - tall
    step = SPAN // down.shape[1]
    for n in range(down_sems.shape[0]):
        for side in range(2):
            pltpu.make_async_copy(
                full.at[side, pl.ds(n * step, step), pl.ds(tall, short), :],
                down.at[pl.ds(n * step, step), pl.ds(side * short, short), :],
                down_sems.at[n],
            ).start()
    both.wait()
    length = rows.shape[0] * rows.shape[1]
    depth = rows.shape[2]
    for g in range(groups):
        many = pl.ds(cuts[g], cuts[g + 1] - cuts[g])
        for side, target in enumerate((gate, up)):
            pltpu.make_async_copy(target.at[:, :, many], target.at[:, :, many], sems.at[g, side]).wait()

        def unit(j, carry):
            lanes = pl.ds(pl.multiple_of(j * 128, 128), 128)
            right = jnp.concatenate(
                [gate[:, :, lanes].reshape(depth, 128), up[:, :, lanes].reshape(depth, 128)], axis=1
            )
            both_sides = dot(rows[...].reshape(length, depth), right)
            g_part, u_part = both_sides[:, :128], both_sides[:, 128:]
            hidden[:, lanes] = (g_part / (1.0 + jnp.exp(-g_part)) * u_part).astype(jnp.bfloat16)
            return carry

        lax.fori_loop(cuts[g] // 128, cuts[g + 1] // 128, unit, 0)
    multiply(tp, hidden, away, mine, down, down_sems, step)


def in_vmem(many):
    return [pl.BlockSpec(memory_space=pltpu.VMEM)] * many


def in_hbm(many):
    return [pl.BlockSpec(memory_space=pltpu.HBM)] * many


def in_smem(many):
    return [pl.BlockSpec(memory_space=pltpu.SMEM)] * many


def retention(place, log_gamma, cosine, sine, gain, own, other, arrays):
    rows, depth = own.shape
    heads = gain.shape[1] // DV
    _, tall, width = arrays[0].shape
    length = 2 * rows
    return pl.pallas_call(
        retention_body,
        in_specs=in_smem(2) + in_vmem(3) + in_hbm(2 + len(arrays)),
        out_specs=pl.BlockSpec(memory_space=pltpu.VMEM),
        out_shape=jax.ShapeDtypeStruct((length, heads * DV), jnp.bfloat16),
        scratch_shapes=[
            pltpu.VMEM((2, rows, depth), jnp.bfloat16),
            pltpu.VMEM((heads, depth // tall, tall, width // heads), jnp.bfloat16),
            pltpu.VMEM((length, DK), jnp.bfloat16),
            pltpu.VMEM((length, DK), jnp.bfloat16),
            pltpu.VMEM((length, DV), jnp.bfloat16),
            pltpu.SemaphoreType.DMA((heads,)),
            pltpu.SemaphoreType.DMA,
        ],
        compiler_params=pltpu.CompilerParams(vmem_limit_bytes=44 * MIB),
        name="retention",
    )(place, log_gamma, cosine, sine, gain, own, other, *arrays)


def project(place, hidden, arrays, depth):
    length, width = hidden.shape
    tall = arrays[0].shape[1]
    half = jax.ShapeDtypeStruct((length // 2, depth), jnp.bfloat16)
    return pl.pallas_call(
        project_body,
        in_specs=in_smem(1) + in_vmem(1) + in_hbm(len(arrays)),
        out_specs=in_vmem(2),
        out_shape=[half, half],
        scratch_shapes=[
            pltpu.VMEM((depth // tall, tall, width), jnp.bfloat16),
            pltpu.SemaphoreType.DMA((depth // SPAN,)),
        ],
        compiler_params=pltpu.CompilerParams(vmem_limit_bytes=32 * MIB),
        name="project",
    )(place, hidden, *arrays)


def feed_forward(place, own, other, full):
    rows, depth = own.shape
    _, shards, tall, units = full.shape
    tall = tall * 2 // 3
    half = jax.ShapeDtypeStruct((rows, depth), jnp.bfloat16)
    return pl.pallas_call(
        feed_forward_body,
        in_specs=in_smem(1) + in_hbm(3),
        out_specs=in_vmem(2),
        out_shape=[half, half],
        scratch_shapes=[
            pltpu.VMEM((2, rows, depth), jnp.bfloat16),
            pltpu.VMEM((shards, tall, units), jnp.bfloat16),
            pltpu.VMEM((shards, tall, units), jnp.bfloat16),
            pltpu.VMEM((2 * rows, units), jnp.bfloat16),
            pltpu.VMEM((shards, tall, units), jnp.bfloat16),
            pltpu.SemaphoreType.DMA,
            pltpu.SemaphoreType.DMA((-(-units // 384), 2)),
            pltpu.SemaphoreType.DMA((depth // SPAN,)),
        ],
        compiler_params=pltpu.CompilerParams(vmem_limit_bytes=52 * MIB),
        name="feed_forward",
    )(place, own, other, full)


def angles(length):
    position = jnp.arange(length, dtype=jnp.float32)
    inverse = 1.0 / rope_base ** jnp.linspace(0.0, 1.0, DK // 2, dtype=jnp.float32)
    angle = position[:, None] * inverse[None, :]
    return jnp.cos(angle), jnp.sin(angle)


def shards(
    resid,
    mix_gain,
    query_weight,
    key_weight,
    value_weight,
    head_gain,
    out_weight,
    mlp_gain,
    gate_weight,
    up_weight,
    down_weight,
):
    rows, depth = resid.shape
    heads = query_weight.shape[1] // DK
    tp = lax.axis_index("tp")
    down_shard = down_weight.T
    tall = down_shard.shape[0]
    mlp_shard = jnp.concatenate(
        [half_of(gate_weight, up_weight), half_of(down_shard[: tall // 2], down_shard[tall // 2 :])], axis=0
    )
    mlp_full = lax.all_gather(mlp_shard, TORUS, axis=0, tiled=True)
    mlp_full = mlp_full.reshape(2, -1, *mlp_shard.shape)

    mixer_shard = jnp.concatenate(
        [
            piece
            for h in range(heads)
            for piece in (
                query_weight[:, h * DK : (h + 1) * DK],
                key_weight[:, h * DK : (h + 1) * DK],
                value_weight[:, h * DV : (h + 1) * DV],
            )
        ],
        axis=1,
    )
    mixer_parts = ring_x_y_z(mixer_shard)
    out_parts = ring_z_y_x(out_weight.T)
    mixer_place = jnp.concatenate([positions(mixer_parts), tp[None]])
    out_place = jnp.concatenate([positions(out_parts), tp[None]])
    head_ids = (tp * heads + jnp.arange(heads, dtype=jnp.int32)).astype(jnp.float32)
    log_gamma = jnp.log1p(-(2.0 ** (-5.0 - 2.0 * head_ids)))
    cosine, sine = angles(2 * rows)

    normed = rms_scale(resid, mix_gain)
    head_out = retention(
        mixer_place, log_gamma, cosine, sine, head_gain[None], normed, swap(normed),
        [array for array, _ in mixer_parts],
    )
    away, mine = project(out_place, head_out, [array for array, _ in out_parts], depth)
    mixer_sum = mine.astype(jnp.float32) + swap(away).astype(jnp.float32)
    middle = (resid.astype(jnp.float32) + mixer_sum).astype(jnp.bfloat16)
    normed_mlp = rms_scale(middle, mlp_gain)
    away, mine = feed_forward(tp[None], normed_mlp, swap(normed_mlp), mlp_full)
    mlp_sum = mine.astype(jnp.float32) + swap(away).astype(jnp.float32)
    return (middle.astype(jnp.float32) + mlp_sum).astype(jnp.bfloat16)


def solution(mesh):
    torus = Mesh(
        mesh.devices.reshape(mesh.shape["rep"], 2, 4, 4, mesh.shape["tp"]),
        ("rep", "fs_0", "fs_1", "fs_2", "tp"),
    )
    return jax.shard_map(
        shards,
        mesh=torus,
        in_specs=(
            P(REP_FS_TP, None),
            P(),
            P(FS, "tp"),
            P(FS, "tp"),
            P(FS, "tp"),
            P("tp"),
            P("tp", FS),
            P(),
            P(FS, "tp"),
            P(FS, "tp"),
            P("tp", FS),
        ),
        out_specs=P(REP_FS_TP, None),
        check_vma=False,
    )
```
